32 devices in a mesh: fs: 16 (over z, y, x), tp: 2 (over core).
Axes of the slice: x: 2, y: 2, z: 4, core: 2. Of those that a mesh axis runs over, the one named last changes fastest.
Arguments:
- tokens: bfloat16 [4096, 2048], P('fs'), may hold values from -6 to 6
- routes: int32 [4096, 6], P('fs'), may hold values from 0 to 15, all different within a row; in each aligned block of 256 rows (0 to 255, 256 to 511, ...) at most 160 rows name the same one
- route_weights: float32 [4096, 6], P('fs'), may hold values from 0.1 to 1
- norm_gain: float32 [2048], P('fs'), may hold values from 0.1 to 1.9
- expert_gate: float32 [16, 2048, 1024], P(None, 'fs', 'tp'), may hold values from -0.125 to 0.125
- expert_up: float32 [16, 2048, 1024], P(None, 'fs', 'tp'), may hold values from -0.125 to 0.125
- expert_down: float32 [16, 2048, 1024], P(None, 'fs', 'tp'), may hold values from -0.1875 to 0.1875
- shared_gate: float32 [2048, 1024], P('fs', 'tp'), may hold values from -0.125 to 0.125
- shared_up: float32 [2048, 1024], P('fs', 'tp'), may hold values from -0.125 to 0.125
- shared_down: float32 [2048, 1024], P('fs', 'tp'), may hold values from -0.1875 to 0.1875
Outputs:
- layer_output: bfloat16 [4096, 2048], P('fs', 'tp')
- sample_gate: bfloat16 [16, 2048, 1024], P('fs', None, 'tp')
- sample_up: bfloat16 [16, 2048, 1024], P('fs', None, 'tp')
- sample_down: bfloat16 [16, 2048, 1024], P('fs', None, 'tp')
- common_gate: bfloat16 [2048, 1024], P(None, 'tp')
- common_up: bfloat16 [2048, 1024], P(None, 'tp')
- common_down: bfloat16 [2048, 1024], P(None, 'tp')
The draws below stay inside these ranges and needn't reach their ends.
Inputs may be any that keep to these rules, and one draw needn't show every extreme that they name: `routes`: each row names 6 different experts. In each aligned block of 256 rows (the rows of one index of fs) no expert is named by more than 160 rows, a bound that some expert reaches in some blocks.
All inputs are finite; a program needn't handle non-finite values.
Results may differ from the reference program's by a relative error of at most 0.015.
Values may be sent and summed in bfloat16 or wider, within the bound.
A program may use at most 128 MiB of HBM per device.

```python
import math
import jax
import jax.numpy as jnp
import numpy as np
from jax import lax

D = 2048
FF = 1024
SH = 1024
TOP = 6
TOK_DEV = 256
EXPERTS = 16
CAP = 160
TOKENS = 4096
N_FS = 16
N_TP = 2


def block_scale(stream_key, dims, split, least, high):
    gain = 1.0
    for dim, blocks in split:
        draws = jax.random.uniform(jax.random.fold_in(jax.random.fold_in(stream_key, 6), dim), (blocks,), jnp.float32, least / len(split), high / len(split))
        gain = gain * jnp.repeat(jnp.exp(draws), dims[dim] // blocks).reshape((-1,) + (1,) * (len(dims) - 1 - dim))
    return gain


def deal_out(key, own, number, rows, count, top, bound, slope):
    ranking = jax.random.permutation(key, count)
    heavy_load, ordinary = shares(count, rows * top, bound, slope, True), shares(count, rows * top, bound, slope, False)
    places = jnp.arange(count)

    def named(tallies, rotation):
        used = int((tallies > 0).sum())
        fixed = max(1, used // 4)
        shifted = fixed + (places - fixed + rotation * (used - fixed)) % max(1, count - fixed)
        return jnp.zeros((count,), jnp.int32).at[ranking[jnp.where(places < fixed, places, shifted)]].set(jnp.asarray(tallies, jnp.int32))

    tallies = jnp.where(number % 4 == 0, named(heavy_load, number // 4), named(ordinary, number - number // 4 - 1))
    mixed = jax.random.permutation(jax.random.fold_in(own, 3), count)
    giver, taker = mixed[0:count // 2 * 2:2], mixed[1:count // 2 * 2:2]
    room = jnp.minimum(tallies[giver] - 1, bound - tallies[taker]) // 2
    room = jnp.where((giver == ranking[0]) | (taker == ranking[0]) | (tallies[taker] == 0), 0, jnp.maximum(room, 0))
    shifted = jax.random.randint(jax.random.fold_in(own, 4), (count // 2,), 0, 1 << 20) % (room + 1)
    tallies = tallies.at[giver].add(-shifted).at[taker].add(shifted)
    items = jnp.searchsorted(jnp.cumsum(tallies), jnp.arange(rows * top), side="right").astype(jnp.int32)
    table = items.reshape(top, rows).T
    table = table[jax.random.permutation(jax.random.fold_in(own, 1), rows)]
    rotation = jax.random.randint(jax.random.fold_in(own, 2), (rows, 1), 0, top)
    return jnp.take_along_axis(table, (jnp.arange(top)[None, :] + rotation) % top, axis=1)


def shares(number_of, total, limit, slope, full):
    portions = [(1 << 20) // math.isqrt(grade ** slope) + 1 for grade in range(1, number_of + 1)]
    largest = limit if full else min(limit, max(-(-total // number_of), total * portions[0] // sum(portions)))
    least = 1 if total - largest >= number_of - 1 else 0
    counts, rest = [largest] + [least] * (number_of - 1), total - largest - least * (number_of - 1)
    while rest > 0:
        free = [i for i in range(1, number_of) if counts[i] < largest] or [i for i in range(1, number_of) if counts[i] < limit]
        pool, budget = sum([portions[i] for i in free]), rest
        for i in free:
            extra = min(limit - counts[i], max(1, budget * portions[i] // pool), rest)
            counts[i] = counts[i] + extra
            rest = rest - extra
    return np.array(counts)


def normal_values(stream_key, shape, scale, limit, shards=(), kind=jnp.bfloat16):
    result = scale * jax.random.normal(stream_key, shape, jnp.float32)
    if shards:
        result = result * block_scale(stream_key, shape, shards, -0.22, 0.18)
    return jnp.clip(result, -limit, limit).astype(kind)


def setup_inputs(seed: int = 0) -> dict:
    streams_of = jax.random.split(jax.random.key(seed), 11)
    tokens = normal_values(streams_of[0], (TOKENS, D), 1.0, 6.0, ((0, 16),))
    routes_keys = jax.random.split(jax.random.fold_in(streams_of[1], 1), TOKENS // TOK_DEV)
    routes_turns = jax.random.permutation(jax.random.fold_in(streams_of[1], 3), TOKENS // TOK_DEV)
    routes = jax.vmap(lambda own, number: deal_out(jax.random.fold_in(streams_of[1], 2), own, number, TOK_DEV, EXPERTS, TOP, CAP, 1))(routes_keys, routes_turns).reshape((TOKENS, TOP))
    route_weights = jnp.clip(jnp.exp(math.log(1.0) - 2.3025851 * jax.random.uniform(streams_of[2], (TOKENS, TOP), jnp.float32) ** block_scale(streams_of[2], (TOKENS, TOP), ((0, 16),), -0.2, 0.2)), 0.1, 1.0)
    norm_gain = jnp.clip(1.0 + 0.18 * jax.random.normal(streams_of[3], (D,), jnp.float32), 0.1, 1.9)
    expert_gate = normal_values(streams_of[4], (EXPERTS, D, FF), D ** -0.5, 0.125, ((1, 16), (2, 2)), jnp.float32)
    expert_up = normal_values(streams_of[5], (EXPERTS, D, FF), D ** -0.5, 0.125, ((1, 16), (2, 2)), jnp.float32)
    expert_down = normal_values(streams_of[6], (EXPERTS, D, FF), FF ** -0.5, 0.1875, ((1, 16), (2, 2)), jnp.float32)
    shared_gate = normal_values(streams_of[7], (D, SH), D ** -0.5, 0.125, ((0, 16), (1, 2)), jnp.float32)
    shared_up = normal_values(streams_of[8], (D, SH), D ** -0.5, 0.125, ((0, 16), (1, 2)), jnp.float32)
    shared_down = normal_values(streams_of[9], (D, SH), SH ** -0.5, 0.1875, ((0, 16), (1, 2)), jnp.float32)
    return dict(tokens=tokens, routes=routes, route_weights=route_weights, norm_gain=norm_gain, expert_gate=expert_gate, expert_up=expert_up, expert_down=expert_down, shared_gate=shared_gate, shared_up=shared_up, shared_down=shared_down)


EPSILON = 1e-06

def normalize(tokens):
    values = tokens.astype(jnp.float32)
    scale = lax.rsqrt(lax.optimization_barrier(jnp.mean(values * values, axis=-1, keepdims=True)) + EPSILON)
    return (values * scale).astype(jnp.bfloat16)

def block_sum(hidden, down):
    block_width = hidden.shape[1] // N_TP
    total = jnp.zeros((hidden.shape[0], down.shape[0]), jnp.float32)
    for block in range(N_TP):
        lower = block * block_width
        part = jnp.dot(hidden[:, lower:lower + block_width], down[:, lower:lower + block_width].T, preferred_element_type=jnp.float32).astype(jnp.bfloat16)
        part = lax.optimization_barrier(part)
        total = total + part.astype(jnp.float32)
    return total

def reference(tokens, routes, route_weights, norm_gain, expert_gate, expert_up, expert_down, shared_gate, shared_up, shared_down):
    sample_gate = (norm_gain[None, :, None] * expert_gate).astype(jnp.bfloat16)
    sample_up = (norm_gain[None, :, None] * expert_up).astype(jnp.bfloat16)
    sample_down = expert_down.astype(jnp.bfloat16)
    common_gate = (norm_gain[:, None] * shared_gate).astype(jnp.bfloat16)
    common_up = (norm_gain[:, None] * shared_up).astype(jnp.bfloat16)
    common_down = shared_down.astype(jnp.bfloat16)
    normed = normalize(tokens)
    route_blocks = routes.reshape(N_FS, TOK_DEV * TOP)
    member = (route_blocks[:, :, None] == jnp.arange(EXPERTS, dtype=jnp.int32)[None, None, :]).astype(jnp.int32)
    before = lax.optimization_barrier(jnp.sum((jnp.cumsum(member, axis=1) - member) * member, axis=2))
    block_index = jnp.arange(N_FS, dtype=jnp.int32)[:, None]
    slots = (route_blocks * (N_FS * CAP) + block_index * CAP + before).reshape(-1)
    row_index = (block_index * TOK_DEV + jnp.arange(TOK_DEV * TOP, dtype=jnp.int32)[None, :] // TOP).reshape(-1)
    sources = jnp.full((EXPERTS * N_FS * CAP,), TOKENS, jnp.int32).at[slots].set(row_index)
    padded = jnp.concatenate([normed, jnp.zeros((1, D), jnp.bfloat16)], axis=0)

    def per_expert(operands):
        expert_rows, gate_w, up_w, down_w = operands
        rows = padded[expert_rows]
        gate = jnp.dot(rows, gate_w, preferred_element_type=jnp.float32)
        upward = jnp.dot(rows, up_w, preferred_element_type=jnp.float32)
        hidden = (jax.nn.silu(gate) * upward).astype(jnp.bfloat16)
        return block_sum(hidden, down_w).astype(jnp.bfloat16)
    expert_out = lax.map(per_expert, (sources.reshape(EXPERTS, N_FS * CAP), sample_gate, sample_up, sample_down))
    picked = expert_out.reshape(EXPERTS * N_FS * CAP, D)[slots].astype(jnp.float32).reshape(TOKENS, TOP, D)
    routed = lax.optimization_barrier(jnp.sum(picked * route_weights[:, :, None], axis=1))
    shared_gate_act = jnp.dot(normed, common_gate, preferred_element_type=jnp.float32)
    shared_up_act = jnp.dot(normed, common_up, preferred_element_type=jnp.float32)
    shared_hidden = (jax.nn.silu(shared_gate_act) * shared_up_act).astype(jnp.bfloat16)
    shared_sum = block_sum(shared_hidden, common_down)
    layer_output = (routed + shared_sum).astype(jnp.bfloat16)
    return (layer_output, sample_gate, sample_up, sample_down, common_gate, common_up, common_down)
```

```python
import jax
import jax.numpy as jnp
from jax import lax
from jax.sharding import PartitionSpec as P

EPSILON = 1e-06


def normalize(tokens):
    values = tokens.astype(jnp.float32)
    scale = lax.rsqrt(jnp.mean(values * values, axis=-1, keepdims=True) + EPSILON)
    return (values * scale).astype(jnp.bfloat16)


def body(
    tokens,
    routes,
    route_weights,
    norm_gain,
    expert_gate,
    expert_up,
    expert_down,
    shared_gate,
    shared_up,
    shared_down,
):
    tp_count = lax.axis_size("tp")
    tp_index = lax.axis_index("tp")
    fs_count = lax.axis_size("fs")
    tok_rows, width = tokens.shape
    experts = expert_gate.shape[0]
    share = tok_rows // tp_count
    own_experts = experts // fs_count

    normed = normalize(tokens)
    own_normed = lax.dynamic_slice_in_dim(normed, tp_index * share, share, 0)
    own_routes = lax.dynamic_slice_in_dim(routes, tp_index * share, share, 0)
    own_weights = lax.dynamic_slice_in_dim(route_weights, tp_index * share, share, 0)
    member = own_routes[None, :, :] == jnp.arange(experts, dtype=jnp.int32)[:, None, None]
    dense = jnp.sum(jnp.where(member, own_weights[None, :, :], 0.0), axis=2)
    gathered = lax.all_gather(own_normed, "fs", axis=0, tiled=True)
    dense_all = lax.all_gather(dense, "fs", axis=0, tiled=False)

    gain_rows = norm_gain[None, :, None]
    rounded = (
        (expert_gate * gain_rows).astype(jnp.bfloat16),
        (expert_up * gain_rows).astype(jnp.bfloat16),
        expert_down.astype(jnp.bfloat16),
    )
    sample_gate, sample_up, sample_down = (
        lax.all_to_all(rounded[0], "fs", split_axis=0, concat_axis=1, tiled=True),
        lax.all_to_all(rounded[1], "fs", split_axis=0, concat_axis=1, tiled=True),
        lax.all_to_all(rounded[2], "fs", split_axis=0, concat_axis=1, tiled=True),
    )

    common_gate, common_up, common_down = (
        lax.all_gather((shared_gate * norm_gain[:, None]).astype(jnp.bfloat16), "fs", axis=0, tiled=True),
        lax.all_gather((shared_up * norm_gain[:, None]).astype(jnp.bfloat16), "fs", axis=0, tiled=True),
        lax.all_gather(shared_down.astype(jnp.bfloat16), "fs", axis=0, tiled=True),
    )
    shared_gate_act = jnp.dot(normed, common_gate, preferred_element_type=jnp.float32)
    shared_up_act = jnp.dot(normed, common_up, preferred_element_type=jnp.float32)
    shared_hidden = (jax.nn.silu(shared_gate_act) * shared_up_act).astype(jnp.bfloat16)
    shared_part = jnp.einsum(
        "th,dh->td", shared_hidden, common_down, preferred_element_type=jnp.float32
    ).astype(jnp.bfloat16)
    shared_parts = lax.all_to_all(
        shared_part.reshape(tok_rows, tp_count, width // tp_count).transpose(1, 0, 2),
        "tp",
        split_axis=0,
        concat_axis=0,
        tiled=True,
    )
    shared_sum = jnp.sum(shared_parts.astype(jnp.float32), axis=0)

    scale_all = lax.dynamic_slice_in_dim(
        dense_all, lax.axis_index("fs") * own_experts, own_experts, 1
    )
    total = None
    for expert in range(own_experts):
        scale = scale_all[:, expert, :].reshape(-1)[:, None]
        for shift in range(tp_count):
            gate_w, up_w, down_w = (
                sample_gate[expert],
                sample_up[expert],
                sample_down[expert],
            )
            if shift:
                ring = [(i, (i + shift) % tp_count) for i in range(tp_count)]
                gate_w, up_w, down_w = (
                    lax.ppermute(gate_w, "tp", ring),
                    lax.ppermute(up_w, "tp", ring),
                    lax.ppermute(down_w, "tp", ring),
                )
            gate = jnp.dot(gathered, gate_w, preferred_element_type=jnp.float32)
            upward = jnp.dot(gathered, up_w, preferred_element_type=jnp.float32)
            hidden = (jax.nn.silu(gate) * upward * scale).astype(jnp.bfloat16)
            part = jnp.einsum("rf,df->rd", hidden, down_w, preferred_element_type=jnp.float32)
            total = part if total is None else total + part
    routed = lax.psum_scatter(
        total.astype(jnp.bfloat16), "fs", scatter_dimension=0, tiled=True
    )
    routed = lax.all_to_all(routed, "tp", split_axis=1, concat_axis=0, tiled=True)
    layer_output = (routed.astype(jnp.float32) + shared_sum).astype(jnp.bfloat16)
    return (layer_output, sample_gate, sample_up, sample_down, common_gate, common_up, common_down)


def solution(mesh):
    return jax.shard_map(
        body,
        mesh=mesh,
        in_specs=(
            P("fs", None),
            P("fs", None),
            P("fs", None),
            P("fs"),
            P(None, "fs", "tp"),
            P(None, "fs", "tp"),
            P(None, "fs", "tp"),
            P("fs", "tp"),
            P("fs", "tp"),
            P("fs", "tp"),
        ),
        out_specs=(
            P("fs", "tp"),
            P("fs", None, "tp"),
            P("fs", None, "tp"),
            P("fs", None, "tp"),
            P(None, "tp"),
            P(None, "tp"),
            P(None, "tp"),
        ),
        check_vma=False,
    )
```

```python
import jax
import jax.numpy as jnp
from jax import lax
from jax.sharding import PartitionSpec as P

EPSILON = 1e-06


def normalize(tokens):
    values = tokens.astype(jnp.float32)
    scale = lax.rsqrt(jnp.mean(values * values, axis=-1, keepdims=True) + EPSILON)
    return (values * scale).astype(jnp.bfloat16)


def ring_of(fs_count):
    if fs_count != 16:
        return list(range(fs_count))
    order = []
    for place, column in enumerate((0, 1, 3, 2)):
        heights = range(4) if place % 2 == 0 else range(3, -1, -1)
        order.extend(height * 4 + column for height in heights)
    return order


def reorder(blocks, order):
    if list(order) == list(range(len(order))):
        return blocks
    return jnp.concatenate([blocks[i : i + 1] for i in order], axis=0)


def body(
    tokens,
    routes,
    route_weights,
    norm_gain,
    expert_gate,
    expert_up,
    expert_down,
    shared_gate,
    shared_up,
    shared_down,
):
    tp_count = lax.axis_size("tp")
    tp_index = lax.axis_index("tp")
    fs_count = lax.axis_size("fs")
    tok_rows, width = tokens.shape
    experts = expert_gate.shape[0]
    share = tok_rows // tp_count
    own_experts = experts // fs_count
    ring = ring_of(fs_count)
    place_of = [ring.index(i) for i in range(fs_count)]
    groups = None if ring == list(range(fs_count)) else [ring]

    normed = normalize(tokens)
    own_normed = lax.dynamic_slice_in_dim(normed, tp_index * share, share, 0)
    own_routes = lax.dynamic_slice_in_dim(routes, tp_index * share, share, 0)
    own_weights = lax.dynamic_slice_in_dim(route_weights, tp_index * share, share, 0)
    member = own_routes[None, :, :] == jnp.arange(experts, dtype=jnp.int32)[:, None, None]
    dense = jnp.sum(jnp.where(member, own_weights[None, :, :], 0.0), axis=2)
    dense_all = lax.all_gather(dense, "fs", axis=0, tiled=False)
    own_normed, dense_all = lax.optimization_barrier((own_normed, dense_all))
    gathered = lax.all_gather(own_normed, "fs", axis=0, tiled=False)
    gathered = reorder(gathered, ring).reshape(fs_count * share, width)

    gain_rows = norm_gain[None, :, None]
    rounded = (
        (expert_gate * gain_rows).astype(jnp.bfloat16),
        (expert_up * gain_rows).astype(jnp.bfloat16),
        expert_down.astype(jnp.bfloat16),
    )
    sample_gate, sample_up, sample_down = (
        lax.all_to_all(rounded[0], "fs", split_axis=0, concat_axis=1, tiled=True),
        lax.all_to_all(rounded[1], "fs", split_axis=0, concat_axis=1, tiled=True),
        lax.all_to_all(rounded[2], "fs", split_axis=0, concat_axis=1, tiled=True),
    )

    half = shared_gate.shape[1]
    shared_rows = jnp.concatenate(
        [
            (shared_gate * norm_gain[:, None]).astype(jnp.bfloat16),
            (shared_up * norm_gain[:, None]).astype(jnp.bfloat16),
            shared_down.astype(jnp.bfloat16),
        ],
        axis=1,
    )
    common = lax.all_gather(shared_rows, "fs", axis=0, tiled=False, axis_index_groups=groups)
    common_gate, common_up, common_down = (
        reorder(common[:, :, i * half : (i + 1) * half], place_of).reshape(width, half)
        for i in range(3)
    )
    shared_gate_act = jnp.dot(normed, common_gate, preferred_element_type=jnp.float32)
    shared_up_act = jnp.dot(normed, common_up, preferred_element_type=jnp.float32)
    shared_hidden = (jax.nn.silu(shared_gate_act) * shared_up_act).astype(jnp.bfloat16)
    shared_part = jnp.einsum(
        "th,dh->td", shared_hidden, common_down, preferred_element_type=jnp.float32
    ).astype(jnp.bfloat16)
    shared_parts = lax.all_to_all(
        shared_part.reshape(tok_rows, tp_count, width // tp_count).transpose(1, 0, 2),
        "tp",
        split_axis=0,
        concat_axis=0,
        tiled=True,
    )
    shared_sum = jnp.sum(shared_parts.astype(jnp.float32), axis=0)

    scale_all = reorder(
        lax.dynamic_slice_in_dim(
            dense_all, lax.axis_index("fs") * own_experts, own_experts, 1
        ),
        ring,
    )
    total = None
    for expert in range(own_experts):
        scale = scale_all[:, expert, :].reshape(-1)[:, None]
        for shift in range(tp_count):
            gate_w, up_w, down_w = (
                sample_gate[expert],
                sample_up[expert],
                sample_down[expert],
            )
            if shift:
                pairs = [(i, (i + shift) % tp_count) for i in range(tp_count)]
                gate_w, up_w, down_w = (
                    lax.ppermute(gate_w, "tp", pairs),
                    lax.ppermute(up_w, "tp", pairs),
                    lax.ppermute(down_w, "tp", pairs),
                )
            gate = jnp.dot(gathered, gate_w, preferred_element_type=jnp.float32)
            upward = jnp.dot(gathered, up_w, preferred_element_type=jnp.float32)
            hidden = (jax.nn.silu(gate) * upward * scale).astype(jnp.bfloat16)
            part = jnp.einsum("rf,df->rd", hidden, down_w, preferred_element_type=jnp.float32)
            total = part if total is None else total + part
    routed = lax.psum_scatter(
        total.astype(jnp.bfloat16), "fs", scatter_dimension=0, tiled=True, axis_index_groups=groups
    )
    routed = lax.all_to_all(routed, "tp", split_axis=1, concat_axis=0, tiled=True)
    layer_output = (routed.astype(jnp.float32) + shared_sum).astype(jnp.bfloat16)
    return (layer_output, sample_gate, sample_up, sample_down, common_gate, common_up, common_down)


def solution(mesh):
    return jax.shard_map(
        body,
        mesh=mesh,
        in_specs=(
            P("fs", None),
            P("fs", None),
            P("fs", None),
            P("fs"),
            P(None, "fs", "tp"),
            P(None, "fs", "tp"),
            P(None, "fs", "tp"),
            P("fs", "tp"),
            P("fs", "tp"),
            P("fs", "tp"),
        ),
        out_specs=(
            P("fs", "tp"),
            P("fs", None, "tp"),
            P("fs", None, "tp"),
            P("fs", None, "tp"),
            P(None, "tp"),
            P(None, "tp"),
            P(None, "tp"),
        ),
        check_vma=False,
    )
```
